32 devices in a mesh: sp: 8 (over z, x), tp: 4 (over y, core).
Axes of the slice: x: 2, y: 2, z: 4, core: 2. Of those that a mesh axis runs over, the one named last changes fastest.
Arguments:
- resid: bfloat16 [4096, 2048], P(('sp', 'tp')), may hold values from -6 to 6
- pool_in: bfloat16 [4096, 1024], P('sp', 'tp'), may hold values from -8 to 8
- doc_ids: int32 [4096], P('sp'), may hold values from 0 to 3, never falling along the last dimension, each value on 1 to 1536 neighbouring positions
- w_group: bfloat16 [8, 128, 128], replicated, may hold values from -0.5 to 0.5
- pool_scale: bfloat16 [1024], replicated, may hold values from 0.099609375 to 1.8984375
- w_branch: bfloat16 [1024, 2048], P('tp'), may hold values from -0.1875 to 0.1875
- norm_gain: bfloat16 [2048], replicated, may hold values from 0.099609375 to 1.8984375
- route_ids: int32 [4096, 4], P(('sp', 'tp')), may hold values from 0 to 31, all different within a row; in each aligned block of 128 rows (0 to 127, 128 to 255, ...) at most 32 rows name the same one
- route_wts: float32 [4096, 4], P(('sp', 'tp')), may hold values from 0.2 to 1
- w_exp_gate: bfloat16 [32, 2048, 512], P(('sp', 'tp')), may hold values from -0.125 to 0.125
- w_exp_up: bfloat16 [32, 2048, 512], P(('sp', 'tp')), may hold values from -0.125 to 0.125
- w_exp_down: bfloat16 [32, 512, 2048], P(('sp', 'tp')), may hold values from -0.25 to 0.25
- w_sh_gate: bfloat16 [2048, 512], replicated, may hold values from -0.125 to 0.125
- w_sh_up: bfloat16 [2048, 512], replicated, may hold values from -0.125 to 0.125
- w_sh_down: bfloat16 [512, 2048], replicated, may hold values from -0.25 to 0.25
- final_gain: bfloat16 [2048], replicated, may hold values from 0.099609375 to 1.8984375
Outputs:
- final: bfloat16 [4096, 2048], P(('sp', 'tp'))
The draws below stay inside these ranges and needn't reach their ends.
Inputs may be any that keep to these rules, and one draw needn't show every extreme that they name: `doc_ids`: never falls along the positions. `route_ids`: each row names 4 different experts; among the rows of one device (aligned blocks of 128 rows) no expert is named by more than 32 rows, a bound that some block reaches.
All inputs are finite; a program needn't handle non-finite values.
Results may differ from the reference program's by a relative error of at most 0.0062.
Values may be sent and summed in bfloat16 or wider, within the bound.
A program may use at most 128 MiB of HBM per device.

```python
import math
import jax
import jax.numpy as jnp
import numpy as np
from jax import lax

D = 2048
GROUP_CH = 128
GROUPS = 8
FF = 512
TOPK = 4
ROWS = 128
P_SIZE = 1024
EXPERTS = 32
TOK_DEV = 512
TOKENS = 4096
CAP = 32
N_SP = 8
DEVICES = 32


def draw_pool_in(key, part):
    offset_key = jax.random.fold_in(key, 11)
    noise_key = jax.random.fold_in(key, 12)
    block_count = TOKENS // 64
    offsets = jnp.clip(jax.random.normal(offset_key, (block_count, P_SIZE), jnp.float32) * 1.5, -4.0, 4.0)
    cell_noise = jnp.clip(jax.random.normal(noise_key, (TOKENS, P_SIZE), jnp.float32), -4.0, 4.0)
    return (jnp.repeat(offsets, 64, axis=0) + cell_noise).astype(jnp.bfloat16)


def block_scale(rng, dims, pieces, least, largest):
    loudness = 1.0
    for axis_at, shards_of in pieces:
        steps = jax.random.uniform(jax.random.fold_in(jax.random.fold_in(rng, 6), axis_at), (shards_of,), jnp.float32, least / len(pieces), largest / len(pieces))
        loudness = loudness * jnp.repeat(jnp.exp(steps), dims[axis_at] // shards_of).reshape((-1,) + (1,) * (len(dims) - 1 - axis_at))
    return loudness


def profile(count, total, bound, skew):
    portions = [(1 << 20) // math.isqrt(standing ** skew) + 1 for standing in range(2, count + 1)]
    rest, given = total - bound - (count - 1), [1] * (count - 1)
    while rest > 0:
        free = [i for i in range(count - 1) if given[i] < bound]
        mass, budget = sum([portions[i] for i in free]), rest
        for i in free:
            more = min(bound - given[i], max(1, budget * portions[i] // mass), rest)
            given[i] = given[i] + more
            rest = rest - more
    return np.array([bound] + given)


def uneven_parts(stream_key, amount, total, reach, lean):
    if amount == 2:
        one = jax.random.randint(stream_key, (), max(1, total - reach), min(reach, total - 1) + 1)
        return jnp.stack([one, total - one])
    sizes = jnp.asarray(profile(amount, total, reach, lean), jnp.int32)
    pairs = (amount - 1) // 2
    donor, receiver = sizes[1:1 + 2 * pairs:2], sizes[2:2 + 2 * pairs:2]
    slack = jnp.minimum(donor - 1, reach - receiver)
    passed = jax.random.randint(jax.random.fold_in(stream_key, 1), (pairs,), 0, 1 << 20) % (slack + 1)
    sizes = sizes.at[1:1 + 2 * pairs:2].set(donor - passed).at[2:2 + 2 * pairs:2].set(receiver + passed)
    return sizes[jax.random.permutation(jax.random.fold_in(stream_key, 2), amount)]


def assign_block(key, own, number, rows, number_of, top, reach, slope):
    sequence = jax.random.permutation(key, number_of)
    packed, common = portions_of(number_of, rows * top, reach, slope, True), portions_of(number_of, rows * top, reach, slope, False)
    places = jnp.arange(number_of)

    def named(sizes, offset_by):
        used = int((sizes > 0).sum())
        fixed = max(1, used // 4)
        passed = fixed + (places - fixed + offset_by * (used - fixed)) % max(1, number_of - fixed)
        return jnp.zeros((number_of,), jnp.int32).at[sequence[jnp.where(places < fixed, places, passed)]].set(jnp.asarray(sizes, jnp.int32))

    sizes = jnp.where(number % 4 == 0, named(packed, number // 4), named(common, number - number // 4 - 1))
    mixed = jax.random.permutation(jax.random.fold_in(own, 3), number_of)
    source_of, taker = mixed[0:number_of // 2 * 2:2], mixed[1:number_of // 2 * 2:2]
    slack = jnp.minimum(sizes[source_of] - 1, reach - sizes[taker]) // 2
    slack = jnp.where((source_of == sequence[0]) | (taker == sequence[0]) | (sizes[taker] == 0), 0, jnp.maximum(slack, 0))
    passed = jax.random.randint(jax.random.fold_in(own, 4), (number_of // 2,), 0, 1 << 20) % (slack + 1)
    sizes = sizes.at[source_of].add(-passed).at[taker].add(passed)
    labels = jnp.searchsorted(jnp.cumsum(sizes), jnp.arange(rows * top), side="right").astype(jnp.int32)
    grid = labels.reshape(top, rows).T
    grid = grid[jax.random.permutation(jax.random.fold_in(own, 1), rows)]
    offset_by = jax.random.randint(jax.random.fold_in(own, 2), (rows, 1), 0, top)
    return jnp.take_along_axis(grid, (jnp.arange(top)[None, :] + offset_by) % top, axis=1)


def portions_of(amount, total, limit, lean, full):
    portions = [(1 << 20) // math.isqrt(standing ** lean) + 1 for standing in range(1, amount + 1)]
    largest = limit if full else min(limit, max(-(-total // amount), total * portions[0] // sum(portions)))
    least = 1 if total - largest >= amount - 1 else 0
    holding, spare = [largest] + [least] * (amount - 1), total - largest - least * (amount - 1)
    while spare > 0:
        free = [i for i in range(1, amount) if holding[i] < largest] or [i for i in range(1, amount) if holding[i] < limit]
        mass, left = sum([portions[i] for i in free]), spare
        for i in free:
            extra = min(limit - holding[i], max(1, left * portions[i] // mass), spare)
            holding[i] = holding[i] + extra
            spare = spare - extra
    return np.array(holding)


def noise(rng, extent, width, bound, shards=(), kind=jnp.bfloat16):
    result = width * jax.random.normal(rng, extent, jnp.float32)
    if shards:
        result = result * block_scale(rng, extent, shards, -0.22, 0.18)
    return jnp.clip(result, -bound, bound).astype(kind)


def setup_inputs(seed: int = 0) -> dict:
    arg_keys = jax.random.split(jax.random.key(seed), 17)
    resid = noise(arg_keys[0], (TOKENS, D), 1.0, 6.0, ((0, 32),))
    pool_in = draw_pool_in(jax.random.fold_in(arg_keys[16], 71), 0)
    doc_ids = jnp.searchsorted(jnp.cumsum(uneven_parts(arg_keys[2], N_SP // 2, TOKENS, 3 * TOK_DEV, 1)), jnp.arange(TOKENS), side="right").astype(jnp.int32)
    w_group = noise(arg_keys[3], (GROUPS, GROUP_CH, GROUP_CH), GROUP_CH ** -0.5, 0.5)
    pool_scale = jnp.clip(1.0 + 0.18 * jax.random.normal(arg_keys[4], (P_SIZE,), jnp.float32), 0.099609375, 1.8984375).astype(jnp.bfloat16)
    w_branch = noise(arg_keys[5], (P_SIZE, D), P_SIZE ** -0.5, 0.1875, ((0, 4),))
    norm_gain = jnp.clip(1.0 + 0.18 * jax.random.normal(arg_keys[6], (D,), jnp.float32), 0.099609375, 1.8984375).astype(jnp.bfloat16)
    route_ids_keys = jax.random.split(jax.random.fold_in(arg_keys[7], 1), TOKENS // ROWS)
    route_ids_turns = jax.random.permutation(jax.random.fold_in(arg_keys[7], 3), TOKENS // ROWS)
    route_ids = jax.vmap(lambda own, number: assign_block(jax.random.fold_in(arg_keys[7], 2), own, number, ROWS, EXPERTS, TOPK, CAP, 2))(route_ids_keys, route_ids_turns).reshape((TOKENS, TOPK))
    route_wts = jnp.clip(0.2 + 0.8 * jax.random.uniform(arg_keys[8], (TOKENS, TOPK), jnp.float32) ** block_scale(arg_keys[8], (TOKENS, TOPK), ((0, 32),), -0.2, 0.2), 0.2, 1.0)
    w_exp_gate = noise(arg_keys[9], (EXPERTS, D, FF), D ** -0.5, 0.125, ((0, 32),))
    w_exp_up = noise(arg_keys[10], (EXPERTS, D, FF), D ** -0.5, 0.125, ((0, 32),))
    w_exp_down = noise(arg_keys[11], (EXPERTS, FF, D), FF ** -0.5, 0.25, ((0, 32),))
    w_sh_gate = noise(arg_keys[12], (D, FF), D ** -0.5, 0.125)
    w_sh_up = noise(arg_keys[13], (D, FF), D ** -0.5, 0.125)
    w_sh_down = noise(arg_keys[14], (FF, D), FF ** -0.5, 0.25)
    final_gain = jnp.clip(1.0 + 0.18 * jax.random.normal(arg_keys[15], (D,), jnp.float32), 0.099609375, 1.8984375).astype(jnp.bfloat16)
    return {"resid": resid, "pool_in": pool_in, "doc_ids": doc_ids, "w_group": w_group, "pool_scale": pool_scale, "w_branch": w_branch, "norm_gain": norm_gain, "route_ids": route_ids, "route_wts": route_wts, "w_exp_gate": w_exp_gate, "w_exp_up": w_exp_up, "w_exp_down": w_exp_down, "w_sh_gate": w_sh_gate, "w_sh_up": w_sh_up, "w_sh_down": w_sh_down, "final_gain": final_gain}


pool_windows = (2, 4, 8, 16, 16, 32, 64, 128)
alpha_mix = 8.0 ** 0.25
norm_eps = 1e-05

def layer_norm(values, scales):
    center = values - lax.optimization_barrier(jnp.mean(values, axis=-1, keepdims=True))
    spread = lax.optimization_barrier(jnp.mean(center * center, axis=-1, keepdims=True))
    return center * lax.rsqrt(spread + norm_eps) * scales.astype(jnp.float32)

def channel_windows(channel_count, group_width):
    groups = jnp.arange(channel_count, dtype=jnp.int32) // group_width
    window_table = jnp.asarray(pool_windows, dtype=jnp.int32)
    matches = groups[:, None] == jnp.arange(len(pool_windows), dtype=jnp.int32)[None, :]
    return lax.optimization_barrier(jnp.sum(jnp.where(matches, window_table[None, :], 0), axis=1)).astype(jnp.float32)

def swiglu_hidden(token_rows, gate_weight, up_weight):
    gate_vals = jnp.dot(token_rows, gate_weight, preferred_element_type=jnp.float32)
    up_vals = jnp.dot(token_rows, up_weight, preferred_element_type=jnp.float32)
    return (jax.nn.silu(gate_vals) * up_vals).astype(jnp.bfloat16)

def reference(resid, pool_in, doc_ids, w_group, pool_scale, w_branch, norm_gain, route_ids, route_wts, w_exp_gate, w_exp_up, w_exp_down, w_sh_gate, w_sh_up, w_sh_down, final_gain):
    values = pool_in.astype(jnp.float32)
    positions = jnp.arange(TOKENS, dtype=jnp.int32)
    change = jnp.concatenate([jnp.ones((1,), bool), doc_ids[1:] != doc_ids[:-1]])
    doc_start = lax.cummax(jnp.where(change, positions, 0), axis=0)
    since_start = (positions - doc_start).astype(jnp.float32)[:, None]
    cumulative = jnp.concatenate([jnp.zeros((1, P_SIZE), jnp.float32), jnp.cumsum(values, axis=0)], axis=0)
    current = cumulative[1:]
    running = current - cumulative[doc_start]
    doc_mean = running / (since_start + 1.0)
    widths = channel_windows(P_SIZE, GROUP_CH)[None, :]
    recent = running
    for window in sorted(set(pool_windows)):
        lagged = jnp.concatenate([jnp.zeros((window - 1, P_SIZE), jnp.float32), cumulative[:TOKENS + 1 - window]], axis=0)
        recent = jnp.where((widths == window) & (since_start >= window), current - lagged, recent)
    window_mean = recent / jnp.minimum(since_start + 1.0, widths)
    offset = (0.5 * (window_mean + doc_mean) - values).astype(jnp.bfloat16)
    mixed_rows = jnp.einsum('tgc,gcd->tgd', offset.reshape(TOKENS, GROUPS, GROUP_CH).astype(jnp.float32), w_group.astype(jnp.float32)).reshape(TOKENS, P_SIZE)
    mixed_rows = (mixed_rows * pool_scale.astype(jnp.float32)).astype(jnp.bfloat16)
    branch = jnp.dot(mixed_rows, w_branch, preferred_element_type=jnp.float32)
    normed = layer_norm(alpha_mix * resid.astype(jnp.float32) + branch, norm_gain).astype(jnp.bfloat16)
    flat_ids = route_ids.reshape(DEVICES, ROWS * TOPK)
    onehot = (flat_ids[:, :, None] == jnp.arange(EXPERTS, dtype=jnp.int32)[None, None, :]).astype(jnp.int32)
    slot_rank = lax.optimization_barrier(jnp.sum(jnp.cumsum(onehot, axis=1) * onehot, axis=2)) - 1
    block_index = jnp.arange(DEVICES, dtype=jnp.int32)[:, None]
    slot_index = (flat_ids * (DEVICES * CAP) + block_index * CAP + slot_rank).reshape(-1)
    assign_total = TOKENS * TOPK
    source = jnp.full((EXPERTS * DEVICES * CAP,), assign_total, jnp.int32)
    source = source.at[slot_index].set(jnp.arange(assign_total, dtype=jnp.int32)).reshape(EXPERTS, DEVICES * CAP)
    padded = jnp.concatenate([normed, jnp.zeros((1, D), jnp.bfloat16)], axis=0)
    weight_pad = jnp.concatenate([route_wts.reshape(-1), jnp.zeros((1,), jnp.float32)])

    def per_expert(accum, inputs):
        assign_ids, gate_weight, up_weight, down_weight = inputs
        token_ids = assign_ids // TOPK
        hidden = swiglu_hidden(padded[token_ids], gate_weight, up_weight)
        expert_out = jnp.dot(hidden, down_weight, preferred_element_type=jnp.float32).astype(jnp.bfloat16)
        scaled = weight_pad[assign_ids][:, None] * expert_out.astype(jnp.float32)
        return (accum.at[token_ids].add(scaled), None)
    routed, _ = lax.scan(per_expert, jnp.zeros((TOKENS + 1, D), jnp.float32), (source, w_exp_gate, w_exp_up, w_exp_down))
    routed = routed[:TOKENS]
    shared = jnp.dot(swiglu_hidden(normed, w_sh_gate, w_sh_up), w_sh_down, preferred_element_type=jnp.float32)
    return layer_norm(alpha_mix * normed.astype(jnp.float32) + routed + shared, final_gain).astype(jnp.bfloat16)
```

```python
import functools

import jax
import jax.numpy as jnp
from jax import lax
from jax.experimental import pallas as pl
from jax.experimental.pallas import tpu as pltpu
from jax.sharding import PartitionSpec as P

pool_windows = (2, 4, 8, 16, 16, 32, 64, 128)
alpha_mix = 8.0**0.25
norm_eps = 1e-05
halo = max(pool_windows)
MESH = pl.DeviceIdType.MESH
wb_chunks = 4
chunks = 4


def layer_norm(values, gain):
    center = values - jnp.mean(values, axis=-1, keepdims=True)
    spread = jnp.mean(center * center, axis=-1, keepdims=True)
    return center * lax.rsqrt(spread + norm_eps) * gain.astype(jnp.float32)


def dot(a, b):
    return jnp.dot(a, b, preferred_element_type=jnp.float32)


def silu_mul(gate, up):
    return (gate / (1.0 + jnp.exp(-gate)) * up).astype(jnp.bfloat16)


def pool_kernel(
    n_sp, n_tp,
    pool_ref, docc_ref, docr_ref, wg_ref, scale_ref, wb_ref, resid_ref, gain_ref, meta_ref,
    out_ref, metas_ref,
    ext, stats, mixed, token_rows, wb_all,
    stat_send, stat_recv, halo_send, halo_recv, mix_send, mix_recv,
    wb_send, wb_recv, fw_send, wb_local,
):
    s, p = lax.axis_index("sp"), lax.axis_index("tp")
    toks, width = pool_ref.shape
    group_width = wg_ref.shape[1]
    rows = resid_ref.shape[0]
    depth = wb_ref.shape[0]
    piece = depth // wb_chunks
    partner = p + 1 - 2 * lax.rem(p, 2)

    barrier = pltpu.get_barrier_semaphore()
    for k in range(1, n_sp):
        pl.semaphore_signal(barrier, inc=1, device_id=(lax.rem(s + k, n_sp), p), device_id_type=MESH)
    for k in range(1, n_tp):
        pl.semaphore_signal(barrier, inc=1, device_id=(s, lax.rem(p + k, n_tp)), device_id_type=MESH)
    pl.semaphore_wait(barrier, n_sp + n_tp - 2)

    def wb_copy(c, src, slot, target, send, recv):
        window = pl.ds(c * piece, piece)
        return pltpu.make_async_remote_copy(
            src_ref=src.at[window], dst_ref=wb_all.at[slot, window],
            send_sem=send, recv_sem=recv, device_id=(s, target), device_id_type=MESH,
        )

    own_wb = pltpu.make_async_copy(wb_ref, wb_all.at[p], wb_local)
    own_wb.start()

    values = pool_ref[...]
    docc, docr = docc_ref[...], docr_ref[...]
    last = jnp.max(docr, axis=1, keepdims=True)
    first = jnp.min(docr, axis=1, keepdims=True).astype(jnp.float32)
    tail = (docr == last).astype(jnp.float32)
    tail_count = jnp.sum(tail, axis=1, keepdims=True)
    sums = dot(jnp.broadcast_to(tail, (8, toks)).astype(jnp.bfloat16), values)
    lane = lax.broadcasted_iota(jnp.int32, (8, 128), 1)
    stats[s, :, 0:width] = sums
    stats[s, :, width + 128 :] = meta_ref[...]
    stats[s, :, width : width + 128] = jnp.where(lane == 0, last.astype(jnp.float32), tail_count)

    halo_copy = pltpu.make_async_remote_copy(
        src_ref=pool_ref.at[pl.ds(toks - halo, halo)], dst_ref=ext.at[pl.ds(0, halo)],
        send_sem=halo_send, recv_sem=halo_recv,
        device_id=(lax.rem(s + 1, n_sp), p), device_id_type=MESH,
    )
    halo_copy.start()
    ext[halo:, :] = values

    tpos = lax.broadcasted_iota(jnp.int32, (toks, toks), 0)
    spos = lax.broadcasted_iota(jnp.int32, (toks, toks), 1)
    same = ((docc == docr) & (spos <= tpos)).astype(jnp.float32)
    here = jnp.sum(same, axis=1, keepdims=True)
    running = dot(same.astype(jnp.bfloat16), values)

    stat_copies = []
    for k in range(1, n_sp):
        stat_copies.append(
            pltpu.make_async_remote_copy(
                src_ref=stats.at[s], dst_ref=stats.at[s],
                send_sem=stat_send.at[k], recv_sem=stat_recv.at[k],
                device_id=(lax.rem(s + k, n_sp), p), device_id_type=MESH,
            )
        )
        stat_copies[-1].start()

    cross = []
    for c in range(wb_chunks):
        for j in range(1, n_tp // 2):
            cross.append(
                wb_copy(c, wb_ref, p, lax.rem(p + 2 * j, n_tp), wb_send.at[j, c], wb_recv.at[2 * j, c])
            )
            cross[-1].start()
    beside = [wb_copy(c, wb_ref, p, partner, wb_send.at[0, c], wb_recv.at[1, c]) for c in range(wb_chunks)]
    for copy in beside:
        copy.start()

    for copy in stat_copies:
        copy.wait_recv()
    prev_count = jnp.zeros((1, 1), jnp.float32)
    prev_sums = jnp.zeros((1, width), jnp.float32)
    for k in range(n_sp):
        block = stats[k]
        joined = (block[0:1, width : width + 1] == first) & (k < s)
        prev_count = prev_count + jnp.where(joined, block[0:1, width + 1 : width + 2], 0.0)
        prev_sums = prev_sums + jnp.where(joined, block[0:1, 0:width], 0.0)
    carried = docc.astype(jnp.float32) == first
    length = here + jnp.where(carried, prev_count, 0.0)
    running = running + jnp.where(carried, prev_sums, 0.0)
    doc_mean = running / length

    halo_copy.wait_recv()
    tpos = lax.broadcasted_iota(jnp.int32, (toks, toks + halo), 0) + halo
    spos = lax.broadcasted_iota(jnp.int32, (toks, toks + halo), 1)
    back = tpos - spos
    groups = width // group_width
    for i in range(groups):
        g = p * groups + i
        window = jnp.int32(0)
        for at, size in enumerate(pool_windows):
            window = jnp.where(g == at, size, window)
        span = jnp.minimum(length, window.astype(jnp.float32))
        band = ((back >= 0) & (back < span.astype(jnp.int32))).astype(jnp.float32).astype(jnp.bfloat16)
        cols = slice(i * group_width, (i + 1) * group_width)
        recent = dot(band, ext[:, cols])
        offset = 0.5 * (recent / span + doc_mean[:, cols]) - values[:, cols].astype(jnp.float32)
        turned = dot(offset.astype(jnp.bfloat16), wg_ref[g])
        scale = scale_ref[0:1, pl.ds(pl.multiple_of(g * group_width, group_width), group_width)]
        mixed[:, cols] = (turned * scale.astype(jnp.float32)).astype(jnp.bfloat16)

    mix_copies = []
    for k in range(1, n_tp):
        q = lax.rem(p + k, n_tp)
        mix_copies.append(
            pltpu.make_async_remote_copy(
                src_ref=mixed.at[pl.ds(pl.multiple_of(q * rows, rows), rows)], dst_ref=token_rows.at[p],
                send_sem=mix_send.at[k], recv_sem=mix_recv.at[k],
                device_id=(s, q), device_id_type=MESH,
            )
        )
        mix_copies[-1].start()
    token_rows[p] = mixed[pl.ds(pl.multiple_of(p * rows, rows), rows), :]

    onward = []
    for c in range(wb_chunks):
        for j in range(1, n_tp // 2):
            slot = lax.rem(p - 2 * j + n_tp, n_tp)
            cross[c * (n_tp // 2 - 1) + j - 1].wait_recv()
            onward.append(
                wb_copy(c, wb_all.at[slot], slot, partner, fw_send.at[j, c], wb_recv.at[2 * j + 1, c])
            )
            onward[-1].start()
    for copy in mix_copies:
        copy.wait_recv()
    own_wb.wait()
    for copy in beside + onward:
        copy.wait_recv()
    branch = alpha_mix * resid_ref[...].astype(jnp.float32)
    for k in range(n_tp):
        branch = branch + dot(token_rows[k], wb_all[k])
    out_ref[...] = layer_norm(branch, gain_ref[...]).astype(jnp.bfloat16)
    metas_ref[...] = stats[:, :, width + 128 :]
    halo_copy.wait_send()
    for copy in stat_copies + mix_copies + cross + beside + onward:
        copy.wait_send()


def expert_kernel(
    n_sp, n_tp, n_x, cap,
    normed_ref, metas_ref, eg_hbm, eu_hbm, ed_hbm, sg_hbm, su_hbm, sd_hbm, gain_ref,
    out_ref,
    eg, eu, ed, sg, su, sd, blocks, outgoing, arrived, returned, column, partial, chain, acc, pick, share,
    load_sem, up_send, down_send, block_recv, go_send, go_recv, back_send, back_recv,
    chain_send, chain_recv,
):
    n_z = n_sp // n_x
    peers = n_x * n_tp
    s, p = lax.axis_index("sp"), lax.axis_index("tp")
    z, x = s // n_x, lax.rem(s, n_x)
    toks, model = normed_ref.shape
    top = metas_ref.shape[1] // 2
    strip = model // chunks

    def mate(q):
        return z * n_x + lax.rem(x + q // n_tp, n_x), lax.rem(p + q % n_tp, n_tp)

    def home(q):
        return z * n_x + lax.rem(x + n_x - q // n_tp, n_x), lax.rem(p + n_tp - q % n_tp, n_tp)

    barrier = pltpu.get_barrier_semaphore()
    for k in range(1, n_z):
        pl.semaphore_signal(barrier, inc=1, device_id=(lax.rem(s + k * n_x, n_sp), p), device_id_type=MESH)
    for q in range(1, peers):
        pl.semaphore_signal(barrier, inc=1, device_id=mate(q), device_id_type=MESH)

    loads = [
        pltpu.make_async_copy(a, b, load_sem.at[i])
        for i, (a, b) in enumerate(
            [(sg_hbm, sg), (su_hbm, su), (sd_hbm, sd), (eg_hbm.at[0], eg), (eu_hbm.at[0], eu), (ed_hbm.at[0], ed)]
        )
    ]
    for load in loads:
        load.start()

    low = jnp.minimum(z, n_z - 1 - z)
    rising = jnp.where(z * 2 < n_z, 1, -1)
    near = [z]
    for i in range(1, n_z):
        swing = z - (i + 1) // 2 if i % 2 else z + i // 2
        near.append(jnp.where(2 * low >= i, swing, z + rising * (i - low)))

    def copy(src, dst, send, recv, where):
        return pltpu.make_async_remote_copy(
            src_ref=src, dst_ref=dst, send_sem=send, recv_sem=recv, device_id=where, device_id_type=MESH
        )

    def lane(c):
        return pl.ds(c * strip, strip)

    above = (jnp.minimum(s + n_x, n_sp - 1), p)
    below = (jnp.maximum(s - n_x, 0), p)

    def up(src, zb, c):
        return copy(src, blocks.at[zb, :, lane(c)], up_send.at[zb, c], block_recv.at[zb, c], above)

    def down(src, zb, c):
        return copy(src, blocks.at[zb, :, lane(c)], down_send.at[zb, c], block_recv.at[zb, c], below)

    def rises(zb):
        return (zb <= z) & (z + 1 < n_z)

    def sinks(zb):
        return (zb >= z) & (z > 0)

    def relay(zb, c):
        src = blocks.at[zb, :, lane(c)]

        @pl.when(rises(zb))
        def _():
            up(src, zb, c).start()

        @pl.when(sinks(zb))
        def _():
            down(src, zb, c).start()

    def receive(i):
        for c in range(chunks):
            up(blocks.at[near[i], :, lane(c)], near[i], c).wait_recv()
            relay(near[i], c)

    def seat(q):
        return pl.ds(q * cap, cap)

    def go(i, q):
        return copy(
            outgoing.at[i, seat(q)], arrived.at[i, seat(q)], go_send.at[i, q], go_recv.at[i, q], mate(q)
        )

    def back(i, q):
        return copy(
            arrived.at[i, seat(q)], returned.at[i, seat(q)], back_send.at[i, q], back_recv.at[i, q], home(q)
        )

    far_first = sorted(range(1, peers), key=lambda q: (q // n_tp == 0) + (q % n_tp == 0))

    def dispatch(i):
        outgoing[i] = dot(pick[near[i]], blocks[near[i]]).astype(jnp.bfloat16)
        for q in far_first:
            go(i, q).start()
        arrived[i, seat(0)] = outgoing[i, seat(0)]

    def experts(i):
        for q in range(1, peers):
            go(i, q).wait_recv()
        tokens = arrived[i]
        inner = silu_mul(dot(tokens, eg[...]), dot(tokens, eu[...]))
        arrived[i] = dot(inner, ed[...]).astype(jnp.bfloat16)
        for q in far_first:
            back(i, q).start()
        returned[i, seat(0)] = arrived[i, seat(0)]

    def combine(i):
        for q in range(1, peers):
            back(i, q).wait_recv()
        both = lax.dot_general(
            share[near[i]], returned[i], (((0,), (0,)), ((), ())), preferred_element_type=jnp.float32
        )
        total = both[0:toks] + both[toks:]
        column[near[i]] = total if i else total + acc[...]

    def link(side, zb, c):
        return copy(
            partial.at[zb, :, lane(c)], chain.at[side, zb, :, lane(c)], chain_send.at[zb, c],
            chain_recv.at[side, zb, c], above if side == 0 else below,
        )

    def take(side, zb, c, holds):
        @pl.when(holds)
        def _():
            link(side, zb, c).wait_recv()
            column[zb, :, lane(c)] += chain[side, zb, :, lane(c)].astype(jnp.float32)

    def pass_on(i):
        zb = near[i]
        for c in range(chunks):
            take(0, zb, c, (zb > z) & (z > 0))
            take(1, zb, c, (zb < z) & (z + 1 < n_z))
            partial[zb, :, lane(c)] = column[zb, :, lane(c)].astype(jnp.bfloat16)

            @pl.when(zb > z)
            def _():
                link(0, zb, c).start()

            @pl.when(zb < z)
            def _():
                link(1, zb, c).start()

    def shared():
        for load in loads[:3]:
            load.wait()
        hidden = silu_mul(dot(normed_ref[...], sg[...]), dot(normed_ref[...], su[...]))
        acc[...] = alpha_mix * normed_ref[...].astype(jnp.float32) + dot(hidden, sd[...])
        for load in loads[3:]:
            load.wait()

    blocks[z] = normed_ref[...]
    pl.semaphore_wait(barrier, n_z + peers - 2)
    for c in range(chunks):
        relay(z, c)

    expert_at = [z * n_x * n_tp + lax.rem(x + q // n_tp, n_x) * n_tp + lax.rem(p + q % n_tp, n_tp) for q in range(peers)]
    earlier = lax.broadcasted_iota(jnp.int32, (toks, toks), 0) < lax.broadcasted_iota(jnp.int32, (toks, toks), 1)
    earlier = earlier.astype(jnp.float32).astype(jnp.bfloat16)
    row = lax.broadcasted_iota(jnp.int32, (peers, toks), 0)
    expert = jnp.zeros((peers, toks), jnp.int32)
    for q in range(peers):
        expert = jnp.where(row == q, expert_at[q], expert)
    expert = expert.astype(jnp.float32)
    slot = lax.broadcasted_iota(jnp.int32, (cap, toks), 0).astype(jnp.float32)

    def plan(i):
        zb = near[i]
        meta = metas_ref[zb * n_x + x]
        chosen = jnp.zeros((peers, toks), jnp.float32)
        weight = jnp.zeros((peers, toks), jnp.float32)
        for a in range(top):
            hit = meta[a : a + 1, :] == expert
            chosen = chosen + jnp.where(hit, 1.0, 0.0)
            weight = weight + jnp.where(hit, meta[top + a : top + a + 1, :], 0.0)
        key = jnp.where(chosen > 0.0, dot(chosen.astype(jnp.bfloat16), earlier), -1.0)
        for q in range(peers):
            taken = slot == key[q : q + 1, :]
            pick[zb, seat(q), :] = jnp.where(taken, 1.0, 0.0).astype(jnp.bfloat16)
            full = jnp.where(taken, weight[q : q + 1, :], 0.0)
            high = full.astype(jnp.bfloat16)
            share[zb, seat(q), 0:toks] = high
            share[zb, seat(q), toks:] = (full - high.astype(jnp.float32)).astype(jnp.bfloat16)

    plan(0)
    dispatch(0)
    for i in range(1, n_z):
        plan(i)
    shared()
    for i in range(1, n_z):
        receive(i)
        dispatch(i)
    last = n_z - 1
    for i in range(last, 0, -1):
        experts(i)
    combine(last)
    pass_on(last)
    experts(0)
    for i in range(last - 1, 0, -1):
        combine(i)
        pass_on(i)
    combine(0)
    for c in range(chunks):
        take(0, z, c, z > 0)
        take(1, z, c, z + 1 < n_z)
    out_ref[...] = layer_norm(column[z], gain_ref[...]).astype(jnp.bfloat16)

    for zb in range(n_z):
        for c in range(chunks):
            src = blocks.at[zb, :, lane(c)]

            @pl.when(rises(zb))
            def _():
                up(src, zb, c).wait_send()

            @pl.when(sinks(zb))
            def _():
                down(src, zb, c).wait_send()

    for i in range(1, n_z):
        for c in range(chunks):
            link(0, near[i], c).wait_send()
    for i in range(n_z):
        for q in range(1, peers):
            go(i, q).wait_send()
            back(i, q).wait_send()


def local(
    n_sp, n_tp,
    resid, pool_in, doc_ids, w_group, pool_scale, w_branch, norm_gain, route_ids, route_wts,
    w_exp_gate, w_exp_up, w_exp_down, w_sh_gate, w_sh_up, w_sh_down, final_gain,
):
    toks, width = pool_in.shape
    rows, model = resid.shape
    depth = w_branch.shape[0]
    cap = 2 * rows * route_ids.shape[1] // (n_sp * n_tp)
    n_x = max(k for k in range(1, n_sp + 1) if n_sp % k == 0 and k * k <= n_sp)
    n_z = n_sp // n_x
    ff = w_sh_gate.shape[1]
    meta = jnp.concatenate([route_ids.astype(jnp.float32), route_wts], axis=1).T
    vmem, hbm = pl.BlockSpec(memory_space=pltpu.VMEM), pl.BlockSpec(memory_space=pl.ANY)
    dma = pltpu.SemaphoreType.DMA
    bf16, f32 = jnp.bfloat16, jnp.float32
    normed, metas = pl.pallas_call(
        functools.partial(pool_kernel, n_sp, n_tp),
        out_shape=(
            jax.ShapeDtypeStruct((rows, model), bf16),
            jax.ShapeDtypeStruct((n_sp, meta.shape[0], rows), f32),
        ),
        in_specs=[vmem] * 5 + [hbm] + [vmem] * 3,
        out_specs=(vmem, vmem),
        scratch_shapes=[
            pltpu.VMEM((halo + toks, width), bf16),
            pltpu.VMEM((n_sp, 8, width + 128 + rows), f32),
            pltpu.VMEM((toks, width), bf16),
            pltpu.VMEM((n_tp, rows, width), bf16),
            pltpu.VMEM((n_tp, depth, model), bf16),
            dma((n_sp,)), dma((n_sp,)), dma, dma, dma((n_tp,)), dma((n_tp,)),
            dma((n_tp, wb_chunks)), dma((n_tp, wb_chunks)), dma((n_tp, wb_chunks)), dma,
        ],
        compiler_params=pltpu.CompilerParams(
            collective_id=0, has_side_effects=True, vmem_limit_bytes=48 << 20
        ),
        name="pool_mixer",
    )(
        pool_in, doc_ids[:, None], doc_ids[None, :], w_group, pool_scale[None, :], w_branch,
        resid, norm_gain[None, :], meta,
    )
    peers = n_x * n_tp
    seats = pltpu.VMEM((n_z, peers * cap, model), bf16)
    block = (rows, model)
    return pl.pallas_call(
        functools.partial(expert_kernel, n_sp, n_tp, n_x, cap),
        out_shape=jax.ShapeDtypeStruct(block, bf16),
        in_specs=[vmem] * 2 + [hbm] * 6 + [vmem],
        out_specs=vmem,
        scratch_shapes=[
            pltpu.VMEM((model, ff), bf16), pltpu.VMEM((model, ff), bf16), pltpu.VMEM((ff, model), bf16),
            pltpu.VMEM((model, ff), bf16), pltpu.VMEM((model, ff), bf16), pltpu.VMEM((ff, model), bf16),
            pltpu.VMEM((n_z, *block), bf16),
            seats, seats, seats,
            pltpu.VMEM((n_z, *block), f32),
            pltpu.VMEM((n_z, *block), bf16),
            pltpu.VMEM((2, n_z, *block), bf16),
            pltpu.VMEM(block, f32),
            pltpu.VMEM((n_z, peers * cap, rows), bf16), pltpu.VMEM((n_z, peers * cap, 2 * rows), bf16),
            dma((6,)), dma((n_z, chunks)), dma((n_z, chunks)), dma((n_z, chunks)),
            dma((n_z, peers)), dma((n_z, peers)), dma((n_z, peers)), dma((n_z, peers)),
            dma((n_z, chunks)), dma((2, n_z, chunks)),
        ],
        compiler_params=pltpu.CompilerParams(
            collective_id=1, has_side_effects=True, vmem_limit_bytes=62 << 20
        ),
        name="routed_experts",
    )(
        normed, metas, w_exp_gate, w_exp_up, w_exp_down,
        w_sh_gate, w_sh_up, w_sh_down, final_gain[None, :],
    )


def solution(mesh):
    both = P(("sp", "tp"), None)
    stack = P(("sp", "tp"), None, None)
    placed = (
        both, P("sp", "tp"), P("sp"), P(), P(), P("tp", None), P(), both, both,
        stack, stack, stack, P(), P(), P(), P(),
    )
    return jax.shard_map(
        functools.partial(local, mesh.shape["sp"], mesh.shape["tp"]),
        mesh=mesh, in_specs=placed, out_specs=both, check_vma=False,
    )
```

```python
import functools

import jax
import jax.numpy as jnp
from jax import lax
from jax.experimental import pallas as pl
from jax.experimental.pallas import tpu as pltpu
from jax.sharding import PartitionSpec as P

pool_windows = (2, 4, 8, 16, 16, 32, 64, 128)
alpha_mix = 8.0**0.25
norm_eps = 1e-05
halo = max(pool_windows)
MESH = pl.DeviceIdType.MESH
wb_cuts = 4
chunks = 4


def layer_norm(values, gain):
    center = values - jnp.mean(values, axis=-1, keepdims=True)
    spread = jnp.mean(center * center, axis=-1, keepdims=True)
    return center * lax.rsqrt(spread + norm_eps) * gain.astype(jnp.float32)


def dot(a, b):
    return jnp.dot(a, b, preferred_element_type=jnp.float32)


def silu_mul(gate, up):
    return (gate / (1.0 + jnp.exp(-gate)) * up).astype(jnp.bfloat16)


def layer_kernel(
    n_sp, n_tp, n_x, cap, top,
    pool_hbm, doc_hbm, wg_hbm, scale_hbm, wb_hbm, resid_hbm, ngain_hbm, ids_hbm, wts_hbm,
    eg_hbm, eu_hbm, ed_hbm, sg_hbm, su_hbm, sd_hbm, fgain_hbm,
    out_ref,
    ext, doc, wg, scales, flat, resid, ngain, ids, wts, fgain,
    stats, mixed, token_rows, wb_all,
    eg, eu, ed, sg, su, sd, blocks, outgoing, arrived, returned, column, partial, chain, acc, pick, share,
    in_sem, stat_send, stat_recv, halo_send, halo_recv, mix_send, mix_recv,
    wby_send, wby_recv, wbx_send, wbx_recv, side_send, side_recv, fw_send, fw_recv,
    load_sem, up_send, down_send, block_recv, go_send, go_recv, back_send, back_recv,
    chain_send, chain_recv,
):
    n_z = n_sp // n_x
    peers = n_x * n_tp
    s, p = lax.axis_index("sp"), lax.axis_index("tp")
    z, x = s // n_x, lax.rem(s, n_x)
    toks, width = mixed.shape
    group_width = wg.shape[1]
    rows, model = resid.shape
    depth = wb_all.shape[1]
    partner = p + 1 - 2 * lax.rem(p, 2)
    strip = model // chunks
    piece = depth // n_x
    cuts = max(1, min(wb_cuts, piece // 32))
    cut = piece // cuts

    def mate(q):
        return z * n_x + lax.rem(x + q // n_tp, n_x), lax.rem(p + q % n_tp, n_tp)

    def home(q):
        return z * n_x + lax.rem(x + n_x - q // n_tp, n_x), lax.rem(p + n_tp - q % n_tp, n_tp)

    barrier = pltpu.get_barrier_semaphore()
    for k in range(1, n_sp):
        pl.semaphore_signal(barrier, inc=1, device_id=(lax.rem(s + k, n_sp), p), device_id_type=MESH)
    for q in range(1, peers):
        if q % n_tp:
            pl.semaphore_signal(barrier, inc=1, device_id=mate(q), device_id_type=MESH)

    inputs = [
        pltpu.make_async_copy(a, b, in_sem.at[i])
        for i, (a, b) in enumerate(
            [
                (wb_hbm, wb_all.at[p]), (pool_hbm, ext.at[pl.ds(halo, toks)]), (doc_hbm, doc), (ids_hbm, ids),
                (wts_hbm, wts), (wg_hbm, wg), (scale_hbm, scales), (resid_hbm, resid), (ngain_hbm, ngain),
                (fgain_hbm, fgain),
            ]
        )
    ]
    for load in inputs:
        load.start()
    loads = [
        pltpu.make_async_copy(a, b, load_sem.at[i])
        for i, (a, b) in enumerate(
            [(sg_hbm, sg), (su_hbm, su), (sd_hbm, sd), (eg_hbm.at[0], eg), (eu_hbm.at[0], eu), (ed_hbm.at[0], ed)]
        )
    ]

    low = jnp.minimum(z, n_z - 1 - z)
    rising = jnp.where(z * 2 < n_z, 1, -1)
    near = [z]
    for i in range(1, n_z):
        swing = z - (i + 1) // 2 if i % 2 else z + i // 2
        near.append(jnp.where(2 * low >= i, swing, z + rising * (i - low)))

    def copy(src, dst, send, recv, where):
        return pltpu.make_async_remote_copy(
            src_ref=src, dst_ref=dst, send_sem=send, recv_sem=recv, device_id=where, device_id_type=MESH
        )

    def lane(c):
        return pl.ds(c * strip, strip)

    above = (jnp.minimum(s + n_x, n_sp - 1), p)
    below = (jnp.maximum(s - n_x, 0), p)

    def up(src, zb, c):
        return copy(src, blocks.at[zb, :, lane(c)], up_send.at[zb, c], block_recv.at[zb, c], above)

    def down(src, zb, c):
        return copy(src, blocks.at[zb, :, lane(c)], down_send.at[zb, c], block_recv.at[zb, c], below)

    def rises(zb):
        return (zb <= z) & (z + 1 < n_z)

    def sinks(zb):
        return (zb >= z) & (z > 0)

    def relay(zb, c):
        src = blocks.at[zb, :, lane(c)]

        @pl.when(rises(zb))
        def _():
            up(src, zb, c).start()

        @pl.when(sinks(zb))
        def _():
            down(src, zb, c).start()

    def receive(i):
        for c in range(chunks):
            up(blocks.at[near[i], :, lane(c)], near[i], c).wait_recv()
            relay(near[i], c)

    def seat(q):
        return pl.ds(q * cap, cap)

    def go(i, q):
        return copy(
            outgoing.at[i, seat(q)], arrived.at[i, seat(q)], go_send.at[i, q], go_recv.at[i, q], mate(q)
        )

    def back(i, q):
        return copy(
            arrived.at[i, seat(q)], returned.at[i, seat(q)], back_send.at[i, q], back_recv.at[i, q], home(q)
        )

    far_first = sorted(range(1, peers), key=lambda q: (q // n_tp == 0) + (q % n_tp == 0))

    def dispatch(i):
        outgoing[i] = dot(pick[near[i]], blocks[near[i]]).astype(jnp.bfloat16)
        for q in far_first:
            go(i, q).start()
        arrived[i, seat(0)] = outgoing[i, seat(0)]

    def experts(i):
        for q in range(1, peers):
            go(i, q).wait_recv()
        tokens = arrived[i]
        inner = silu_mul(dot(tokens, eg[...]), dot(tokens, eu[...]))
        arrived[i] = dot(inner, ed[...]).astype(jnp.bfloat16)
        for q in far_first:
            back(i, q).start()
        returned[i, seat(0)] = arrived[i, seat(0)]

    def combine(i):
        for q in range(1, peers):
            back(i, q).wait_recv()
        both = lax.dot_general(
            share[near[i]], returned[i], (((0,), (0,)), ((), ())), preferred_element_type=jnp.float32
        )
        total = both[0:rows] + both[rows:]
        column[near[i]] = total if i else total + acc[...]

    def link(side, zb, c):
        return copy(
            partial.at[zb, :, lane(c)], chain.at[side, zb, :, lane(c)], chain_send.at[zb, c],
            chain_recv.at[side, zb, c], above if side == 0 else below,
        )

    def take(side, zb, c, holds):
        @pl.when(holds)
        def _():
            link(side, zb, c).wait_recv()
            column[zb, :, lane(c)] += chain[side, zb, :, lane(c)].astype(jnp.float32)

    def pass_on(i):
        zb = near[i]
        for c in range(chunks):
            take(0, zb, c, (zb > z) & (z > 0))
            take(1, zb, c, (zb < z) & (z + 1 < n_z))
            partial[zb, :, lane(c)] = column[zb, :, lane(c)].astype(jnp.bfloat16)

            @pl.when(zb > z)
            def _():
                link(0, zb, c).start()

            @pl.when(zb < z)
            def _():
                link(1, zb, c).start()

    def shared():
        for load in loads[:3]:
            load.wait()
        hidden = silu_mul(dot(blocks[z], sg[...]), dot(blocks[z], su[...]))
        acc[...] = alpha_mix * blocks[z].astype(jnp.float32) + dot(hidden, sd[...])
        for load in loads[3:]:
            load.wait()


    def wb_rows(at, c):
        return pl.ds(pl.multiple_of(at * piece + c * cut, cut), cut)

    def wb_copy(slot, at, c, send, recv, where):
        src = wb_all.at[slot, wb_rows(at, c)]
        return copy(src, src, send, recv, where)

    def across(j, c):
        return wb_copy(p, x, c, wby_send.at[j, c], wby_recv.at[j, c], (s, lax.rem(p + 2 * j, n_tp)))

    def slot_of(j):
        return lax.rem(p - 2 * j + n_tp, n_tp)

    def along(j, o, c):
        where = (z * n_x + lax.rem(x + o, n_x), p)
        return wb_copy(slot_of(j), x, c, wbx_send.at[j, o, c], wbx_recv.at[j, o, c], where)

    def onward(j, o, c):
        at = lax.rem(x + n_x - o, n_x)
        return wb_copy(slot_of(j), at, c, fw_send.at[j, o, c], fw_recv.at[j, o, c], (s, partner))

    steps = range(1, n_tp // 2)

    def spread(c):
        for j in steps:
            across(j, c).wait_recv()
            for o in range(1, n_x):
                along(j, o, c).start()
            onward(j, 0, c).start()

    def gather(c):
        for j in steps:
            for o in range(1, n_x):
                along(j, o, c).wait_recv()
                onward(j, o, c).start()

    side = copy(wb_all.at[p], wb_all.at[p], side_send, side_recv, (s, partner))
    halo_copy = copy(
        ext.at[pl.ds(toks, halo)], ext.at[pl.ds(0, halo)], halo_send, halo_recv, (lax.rem(s + 1, n_sp), p)
    )
    stat_copies = [
        copy(stats.at[s], stats.at[s], stat_send.at[k], stat_recv.at[k], (lax.rem(s + k, n_sp), p))
        for k in range(1, n_sp)
    ]
    inputs[0].wait()
    pl.semaphore_wait(barrier, n_sp - 1 + n_x * (n_tp - 1))
    for c in range(cuts):
        for j in steps:
            across(j, c).start()
    side.start()
    for load in inputs[1:5]:
        load.wait()
    halo_copy.start()

    values = ext[halo:, :]
    docr = doc[...][None, :]
    docc = jnp.transpose(jnp.broadcast_to(docr.astype(jnp.float32), (128, toks)))[:, 0:1]
    docr = docr.astype(jnp.float32)
    last = jnp.max(docr, axis=1, keepdims=True)
    first = jnp.min(docr, axis=1, keepdims=True)
    tail = (docr == last).astype(jnp.float32)
    tail_count = jnp.sum(tail, axis=1, keepdims=True)
    sums = dot(jnp.broadcast_to(tail, (8, toks)).astype(jnp.bfloat16), values)
    lane_at = lax.broadcasted_iota(jnp.int32, (8, 128), 1)
    stats[s, :, 0:width] = sums
    stats[s, 0:top, width + 128 :] = ids[...].astype(jnp.float32)
    stats[s, top : 2 * top, width + 128 :] = wts[...]
    stats[s, :, width : width + 128] = jnp.where(lane_at == 0, last, tail_count)
    for each in stat_copies:
        each.start()
    for load in loads:
        load.start()

    tpos = lax.broadcasted_iota(jnp.int32, (toks, toks), 0)
    spos = lax.broadcasted_iota(jnp.int32, (toks, toks), 1)
    same = ((docc == docr) & (spos <= tpos)).astype(jnp.float32)
    here = jnp.sum(same, axis=1, keepdims=True)
    running = dot(same.astype(jnp.bfloat16), values)
    spread(0)

    for each in stat_copies:
        each.wait_recv()
    prev_count = jnp.zeros((1, 1), jnp.float32)
    prev_sums = jnp.zeros((1, width), jnp.float32)
    for k in range(n_sp):
        block = stats[k]
        joined = (block[0:1, width : width + 1] == first) & (k < s)
        prev_count = prev_count + jnp.where(joined, block[0:1, width + 1 : width + 2], 0.0)
        prev_sums = prev_sums + jnp.where(joined, block[0:1, 0:width], 0.0)
    carried = docc == first
    length = here + jnp.where(carried, prev_count, 0.0)
    running = running + jnp.where(carried, prev_sums, 0.0)
    doc_mean = running / length

    halo_copy.wait_recv()
    for load in inputs[5:]:
        load.wait()
    if cuts > 1:
        spread(1)
    tpos = lax.broadcasted_iota(jnp.int32, (toks, toks + halo), 0) + halo
    spos = lax.broadcasted_iota(jnp.int32, (toks, toks + halo), 1)
    away = tpos - spos
    groups = width // group_width
    flat[...] = scales[...].astype(jnp.float32)[None, :]
    for i in range(groups):
        g = p * groups + i
        window = jnp.int32(0)
        for at, size in enumerate(pool_windows):
            window = jnp.where(g == at, size, window)
        span = jnp.minimum(length, window.astype(jnp.float32))
        band = ((away >= 0) & (away < span.astype(jnp.int32))).astype(jnp.float32).astype(jnp.bfloat16)
        cols = slice(i * group_width, (i + 1) * group_width)
        recent = dot(band, ext[:, cols])
        offset = 0.5 * (recent / span + doc_mean[:, cols]) - values[:, cols].astype(jnp.float32)
        turned = dot(offset.astype(jnp.bfloat16), wg[g])
        scale = flat[0:1, pl.ds(pl.multiple_of(g * group_width, group_width), group_width)]
        mixed[:, cols] = (turned * scale).astype(jnp.bfloat16)

    mix_copies = []
    for k in range(1, n_tp):
        q = lax.rem(p + k, n_tp)
        mix_copies.append(
            copy(
                mixed.at[pl.ds(pl.multiple_of(q * rows, rows), rows)], token_rows.at[p],
                mix_send.at[k], mix_recv.at[k], (s, q),
            )
        )
        mix_copies[-1].start()
    token_rows[p] = mixed[pl.ds(pl.multiple_of(p * rows, rows), rows), :]
    for c in range(2, cuts):
        spread(c)
        gather(c - 2)

    expert_at = [z * n_x * n_tp + lax.rem(x + q // n_tp, n_x) * n_tp + lax.rem(p + q % n_tp, n_tp) for q in range(peers)]
    earlier = lax.broadcasted_iota(jnp.int32, (rows, rows), 0) < lax.broadcasted_iota(jnp.int32, (rows, rows), 1)
    earlier = earlier.astype(jnp.float32).astype(jnp.bfloat16)
    row = lax.broadcasted_iota(jnp.int32, (peers, rows), 0)
    expert = jnp.zeros((peers, rows), jnp.int32)
    for q in range(peers):
        expert = jnp.where(row == q, expert_at[q], expert)
    expert = expert.astype(jnp.float32)
    slot = lax.broadcasted_iota(jnp.int32, (cap, rows), 0).astype(jnp.float32)

    def plan(i):
        zb = near[i]
        meta = stats[zb * n_x + x, :, width + 128 :]
        chosen = jnp.zeros((peers, rows), jnp.float32)
        weight = jnp.zeros((peers, rows), jnp.float32)
        for a in range(top):
            hit = meta[a : a + 1, :] == expert
            chosen = chosen + jnp.where(hit, 1.0, 0.0)
            weight = weight + jnp.where(hit, meta[top + a : top + a + 1, :], 0.0)
        key = jnp.where(chosen > 0.0, dot(chosen.astype(jnp.bfloat16), earlier), -1.0)
        for q in range(peers):
            taken = slot == key[q : q + 1, :]
            pick[zb, seat(q), :] = jnp.where(taken, 1.0, 0.0).astype(jnp.bfloat16)
            full = jnp.where(taken, weight[q : q + 1, :], 0.0)
            high = full.astype(jnp.bfloat16)
            share[zb, seat(q), 0:rows] = high
            share[zb, seat(q), rows:] = (full - high.astype(jnp.float32)).astype(jnp.bfloat16)

    plan(0)
    if cuts > 1:
        gather(cuts - 2)
    for i in range(1, n_z):
        plan(i)
    gather(cuts - 1)
    for each in mix_copies:
        each.wait_recv()
    side.wait_recv()
    branch = alpha_mix * resid[...].astype(jnp.float32)
    for k in (p, partner):
        branch = branch + dot(token_rows[k], wb_all[k])
    for c in range(cuts):
        for j in steps:
            for o in range(n_x):
                onward(j, o, c).wait_recv()
    for j in steps:
        for k in (slot_of(j), partner + slot_of(j) - p):
            branch = branch + dot(token_rows[k], wb_all[k])
    blocks[z] = layer_norm(branch, ngain[...][None, :]).astype(jnp.bfloat16)
    for c in range(chunks):
        relay(z, c)

    dispatch(0)
    shared()
    for i in range(1, n_z):
        receive(i)
        dispatch(i)
    last = n_z - 1
    for i in range(last, 0, -1):
        experts(i)
    combine(last)
    pass_on(last)
    experts(0)
    for i in range(last - 1, 0, -1):
        combine(i)
        pass_on(i)
    combine(0)
    for c in range(chunks):
        take(0, z, c, z > 0)
        take(1, z, c, z + 1 < n_z)
    out_ref[...] = layer_norm(column[z], fgain[...][None, :]).astype(jnp.bfloat16)

    for zb in range(n_z):
        for c in range(chunks):
            src = blocks.at[zb, :, lane(c)]

            @pl.when(rises(zb))
            def _():
                up(src, zb, c).wait_send()

            @pl.when(sinks(zb))
            def _():
                down(src, zb, c).wait_send()

    for i in range(1, n_z):
        for c in range(chunks):
            link(0, near[i], c).wait_send()
    for i in range(n_z):
        for q in range(1, peers):
            go(i, q).wait_send()
            back(i, q).wait_send()
    halo_copy.wait_send()
    side.wait_send()
    for each in stat_copies + mix_copies:
        each.wait_send()
    for c in range(cuts):
        for j in steps:
            across(j, c).wait_send()
            onward(j, 0, c).wait_send()
            for o in range(1, n_x):
                along(j, o, c).wait_send()
                onward(j, o, c).wait_send()


def local(
    n_sp, n_tp,
    resid, pool_in, doc_ids, w_group, pool_scale, w_branch, norm_gain, route_ids, route_wts,
    w_exp_gate, w_exp_up, w_exp_down, w_sh_gate, w_sh_up, w_sh_down, final_gain,
):
    toks, width = pool_in.shape
    rows, model = resid.shape
    depth = w_branch.shape[0]
    top = route_ids.shape[1]
    cap = 2 * rows * top // (n_sp * n_tp)
    n_x = max(k for k in range(1, n_sp + 1) if n_sp % k == 0 and k * k <= n_sp)
    n_z = n_sp // n_x
    ff = w_sh_gate.shape[1]
    vmem, hbm = pl.BlockSpec(memory_space=pltpu.VMEM), pl.BlockSpec(memory_space=pl.ANY)
    dma = pltpu.SemaphoreType.DMA
    bf16, f32 = jnp.bfloat16, jnp.float32
    peers = n_x * n_tp
    seats = pltpu.VMEM((n_z, peers * cap, model), bf16)
    block = (rows, model)
    wide, tall = pltpu.VMEM((model, ff), bf16), pltpu.VMEM((ff, model), bf16)
    hops = n_tp // 2
    return pl.pallas_call(
        functools.partial(layer_kernel, n_sp, n_tp, n_x, cap, top),
        out_shape=jax.ShapeDtypeStruct(block, bf16),
        in_specs=[hbm] * 16,
        out_specs=vmem,
        scratch_shapes=[
            pltpu.VMEM((halo + toks, width), bf16),
            pltpu.VMEM(doc_ids.shape, jnp.int32),
            pltpu.VMEM(w_group.shape, bf16),
            pltpu.VMEM(pool_scale.shape, bf16),
            pltpu.VMEM((1, *pool_scale.shape), f32),
            pltpu.VMEM(block, bf16),
            pltpu.VMEM((model,), bf16),
            pltpu.VMEM((top, rows), jnp.int32),
            pltpu.VMEM((top, rows), f32),
            pltpu.VMEM((model,), bf16),
            pltpu.VMEM((n_sp, 8, width + 128 + rows), f32),
            pltpu.VMEM((toks, width), bf16),
            pltpu.VMEM((n_tp, rows, width), bf16),
            pltpu.VMEM((n_tp, depth, model), bf16),
            wide, wide, tall, wide, wide, tall,
            pltpu.VMEM((n_z, *block), bf16),
            seats, seats, seats,
            pltpu.VMEM((n_z, *block), f32),
            pltpu.VMEM((n_z, *block), bf16),
            pltpu.VMEM((2, n_z, *block), bf16),
            pltpu.VMEM(block, f32),
            pltpu.VMEM((n_z, peers * cap, rows), bf16), pltpu.VMEM((n_z, peers * cap, 2 * rows), bf16),
            dma((10,)), dma((n_sp,)), dma((n_sp,)), dma, dma, dma((n_tp,)), dma((n_tp,)),
            dma((hops, wb_cuts)), dma((hops, wb_cuts)),
            dma((hops, n_x, wb_cuts)), dma((hops, n_x, wb_cuts)), dma, dma,
            dma((hops, n_x, wb_cuts)), dma((hops, n_x, wb_cuts)),
            dma((6,)), dma((n_z, chunks)), dma((n_z, chunks)), dma((n_z, chunks)),
            dma((n_z, peers)), dma((n_z, peers)), dma((n_z, peers)), dma((n_z, peers)),
            dma((n_z, chunks)), dma((2, n_z, chunks)),
        ],
        compiler_params=pltpu.CompilerParams(
            collective_id=0, has_side_effects=True, vmem_limit_bytes=62 << 20
        ),
        name="pool_and_experts",
    )(
        pool_in, doc_ids, w_group, pool_scale, w_branch, resid, norm_gain, route_ids.T, route_wts.T,
        w_exp_gate, w_exp_up, w_exp_down, w_sh_gate, w_sh_up, w_sh_down, final_gain,
    )


def solution(mesh):
    both = P(("sp", "tp"), None)
    stack = P(("sp", "tp"), None, None)
    placed = (
        both, P("sp", "tp"), P("sp"), P(), P(), P("tp", None), P(), both, both,
        stack, stack, stack, P(), P(), P(), P(),
    )
    return jax.shard_map(
        functools.partial(local, mesh.shape["sp"], mesh.shape["tp"]),
        mesh=mesh, in_specs=placed, out_specs=both, check_vma=False,
    )
```

```python
import functools

import jax
import jax.numpy as jnp
from jax import lax
from jax.experimental import pallas as pl
from jax.experimental.pallas import tpu as pltpu
from jax.sharding import PartitionSpec as P

pool_windows = (2, 4, 8, 16, 16, 32, 64, 128)
alpha_mix = 8.0**0.25
norm_eps = 1e-05
halo = max(pool_windows)
MESH = pl.DeviceIdType.MESH
wb_cuts = 4
sent_part = 4 / 8
chunks = 4


def layer_norm(values, gain):
    center = values - jnp.mean(values, axis=-1, keepdims=True)
    spread = jnp.mean(center * center, axis=-1, keepdims=True)
    return center * lax.rsqrt(spread + norm_eps) * gain.astype(jnp.float32)


def dot(a, b):
    return jnp.dot(a, b, preferred_element_type=jnp.float32)


def silu_mul(gate, up):
    return (gate / (1.0 + jnp.exp(-gate)) * up).astype(jnp.bfloat16)


def layer_kernel(
    n_sp, n_tp, n_x, cap, top,
    pool_hbm, doc_hbm, wg_hbm, scale_hbm, wb_hbm, resid_hbm, ngain_hbm, ids_hbm, wts_hbm,
    eg_hbm, eu_hbm, ed_hbm, sg_hbm, su_hbm, sd_hbm, fgain_hbm,
    out_ref,
    ext, doc, docx, wg, scales, flat, resid, ngain, ids, wts, fgain,
    stats, mixed, token_rows, wb_all, lent, parts_out, parts_in,
    eg, eu, ed, sg, su, sd, blocks, outgoing, arrived, returned, column, partial, chain, acc, pick, share,
    in_sem, stat_send, stat_recv, halo_send, halo_recv, doc_send, doc_recv, mix_send, mix_recv,
    wby_send, wby_recv, wbx_send, wbx_recv, side_send, side_recv, fw_send, fw_recv,
    lent_send, lent_recv, part_send, part_recv,
    load_sem, up_send, down_send, block_recv, go_send, go_recv, back_send, back_recv,
    chain_send, chain_recv,
):
    n_z = n_sp // n_x
    peers = n_x * n_tp
    s, p = lax.axis_index("sp"), lax.axis_index("tp")
    z, x = s // n_x, lax.rem(s, n_x)
    toks, width = mixed.shape
    group_width = wg.shape[1]
    rows, model = resid.shape
    depth = wb_all.shape[1]
    partner = p + 1 - 2 * lax.rem(p, 2)
    strip = model // chunks
    piece = depth // n_x
    cuts = max(1, min(wb_cuts, piece // 32))
    cut = piece // cuts
    kept = model - parts_in.shape[2]

    def mate(q):
        return z * n_x + lax.rem(x + q // n_tp, n_x), lax.rem(p + q % n_tp, n_tp)

    def home(q):
        return z * n_x + lax.rem(x + n_x - q // n_tp, n_x), lax.rem(p + n_tp - q % n_tp, n_tp)

    barrier = pltpu.get_barrier_semaphore()
    for k in range(1, n_sp):
        pl.semaphore_signal(barrier, inc=1, device_id=(lax.rem(s + k, n_sp), p), device_id_type=MESH)
    for q in range(1, peers):
        if q % n_tp:
            pl.semaphore_signal(barrier, inc=1, device_id=mate(q), device_id_type=MESH)

    inputs = [
        pltpu.make_async_copy(a, b, in_sem.at[i])
        for i, (a, b) in enumerate(
            [
                (wb_hbm, wb_all.at[p]), (pool_hbm, ext.at[pl.ds(halo, toks)]), (doc_hbm, doc), (ids_hbm, ids),
                (wts_hbm, wts), (wg_hbm, wg), (scale_hbm, scales), (resid_hbm, resid), (ngain_hbm, ngain),
                (fgain_hbm, fgain),
            ]
        )
    ]
    for load in inputs:
        load.start()
    loads = [
        pltpu.make_async_copy(a, b, load_sem.at[i])
        for i, (a, b) in enumerate(
            [(sg_hbm, sg), (su_hbm, su), (sd_hbm, sd), (eg_hbm.at[0], eg), (eu_hbm.at[0], eu), (ed_hbm.at[0], ed)]
        )
    ]

    low = jnp.minimum(z, n_z - 1 - z)
    rising = jnp.where(z * 2 < n_z, 1, -1)
    near = [z]
    for i in range(1, n_z):
        swing = z - (i + 1) // 2 if i % 2 else z + i // 2
        near.append(jnp.where(2 * low >= i, swing, z + rising * (i - low)))

    def copy(src, dst, send, recv, where):
        return pltpu.make_async_remote_copy(
            src_ref=src, dst_ref=dst, send_sem=send, recv_sem=recv, device_id=where, device_id_type=MESH
        )

    def lane(c):
        return pl.ds(c * strip, strip)

    above = (jnp.minimum(s + n_x, n_sp - 1), p)
    below = (jnp.maximum(s - n_x, 0), p)

    def up(src, zb, c):
        return copy(src, blocks.at[zb, :, lane(c)], up_send.at[zb, c], block_recv.at[zb, c], above)

    def down(src, zb, c):
        return copy(src, blocks.at[zb, :, lane(c)], down_send.at[zb, c], block_recv.at[zb, c], below)

    def rises(zb):
        return (zb <= z) & (z + 1 < n_z)

    def sinks(zb):
        return (zb >= z) & (z > 0)

    def relay(zb, c):
        src = blocks.at[zb, :, lane(c)]

        @pl.when(rises(zb))
        def _():
            up(src, zb, c).start()

        @pl.when(sinks(zb))
        def _():
            down(src, zb, c).start()

    def receive(i):
        for c in range(chunks):
            up(blocks.at[near[i], :, lane(c)], near[i], c).wait_recv()
            relay(near[i], c)

    def seat(q):
        return pl.ds(q * cap, cap)

    def go(i, q):
        return copy(
            outgoing.at[i, seat(q)], arrived.at[i, seat(q)], go_send.at[i, q], go_recv.at[i, q], mate(q)
        )

    def back(i, q):
        return copy(
            arrived.at[i, seat(q)], returned.at[i, seat(q)], back_send.at[i, q], back_recv.at[i, q], home(q)
        )

    far_first = sorted(range(1, peers), key=lambda q: (q // n_tp == 0) + (q % n_tp == 0))

    def dispatch(i):
        outgoing[i] = dot(pick[near[i]], blocks[near[i]]).astype(jnp.bfloat16)
        for q in far_first:
            go(i, q).start()
        arrived[i, seat(0)] = outgoing[i, seat(0)]

    def experts(i):
        for q in range(1, peers):
            go(i, q).wait_recv()
        tokens = arrived[i]
        inner = silu_mul(dot(tokens, eg[...]), dot(tokens, eu[...]))
        arrived[i] = dot(inner, ed[...]).astype(jnp.bfloat16)
        for q in far_first:
            back(i, q).start()
        returned[i, seat(0)] = arrived[i, seat(0)]

    def combine(i):
        for q in range(1, peers):
            back(i, q).wait_recv()
        both = lax.dot_general(
            share[near[i]], returned[i], (((0,), (0,)), ((), ())), preferred_element_type=jnp.float32
        )
        total = both[0:rows] + both[rows:]
        column[near[i]] = total if i else total + acc[...]

    def link(side, zb, c):
        return copy(
            partial.at[zb, :, lane(c)], chain.at[side, zb, :, lane(c)], chain_send.at[zb, c],
            chain_recv.at[side, zb, c], above if side == 0 else below,
        )

    def take(side, zb, c, holds):
        @pl.when(holds)
        def _():
            link(side, zb, c).wait_recv()
            column[zb, :, lane(c)] += chain[side, zb, :, lane(c)].astype(jnp.float32)

    def pass_on(i):
        zb = near[i]
        for c in range(chunks):
            take(0, zb, c, (zb > z) & (z > 0))
            take(1, zb, c, (zb < z) & (z + 1 < n_z))
            partial[zb, :, lane(c)] = column[zb, :, lane(c)].astype(jnp.bfloat16)

            @pl.when(zb > z)
            def _():
                link(0, zb, c).start()

            @pl.when(zb < z)
            def _():
                link(1, zb, c).start()

    def shared():
        for load in loads[:3]:
            load.wait()
        hidden = silu_mul(dot(blocks[z], sg[...]), dot(blocks[z], su[...]))
        acc[...] = alpha_mix * blocks[z].astype(jnp.float32) + dot(hidden, sd[...])
        for load in loads[3:]:
            load.wait()


    def wb_rows(at, c):
        return pl.ds(pl.multiple_of(at * piece + c * cut, cut), cut)

    def wb_copy(slot, at, c, send, recv, where):
        src = wb_all.at[slot, wb_rows(at, c), pl.ds(0, kept)]
        return copy(src, src, send, recv, where)

    def across(j, c):
        return wb_copy(p, x, c, wby_send.at[j, c], wby_recv.at[j, c], (s, lax.rem(p + 2 * j, n_tp)))

    def slot_of(j):
        return lax.rem(p - 2 * j + n_tp, n_tp)

    def along(j, o, c):
        where = (z * n_x + lax.rem(x + o, n_x), p)
        return wb_copy(slot_of(j), x, c, wbx_send.at[j, o, c], wbx_recv.at[j, o, c], where)

    def onward(j, o, c):
        at = lax.rem(x + n_x - o, n_x)
        return wb_copy(slot_of(j), at, c, fw_send.at[j, o, c], fw_recv.at[j, o, c], (s, partner))

    steps = range(1, n_tp // 2)

    def spread(c):
        if c >= cuts:
            return
        for j in steps:
            across(j, c).wait_recv()
            for o in range(1, n_x):
                along(j, o, c).start()
            onward(j, 0, c).start()

    def gather(c):
        if not 0 <= c < cuts:
            return
        for j in steps:
            for o in range(1, n_x):
                along(j, o, c).wait_recv()
                onward(j, o, c).start()

    def block_rows(q):
        return pl.ds(pl.multiple_of(q * rows, rows), rows)

    def lend(j):
        q = lax.rem(partner + 2 * j, n_tp)
        return copy(mixed.at[block_rows(q)], lent.at[j], lent_send.at[j], lent_recv.at[j], (s, partner))

    def part(j):
        return copy(
            parts_out.at[j], parts_in.at[j], part_send.at[j], part_recv.at[j], (s, lax.rem(p + 2 * j, n_tp))
        )

    side = copy(wb_all.at[p], wb_all.at[p], side_send, side_recv, (s, partner))
    halo_copy = copy(
        ext.at[pl.ds(toks, halo)], ext.at[pl.ds(0, halo)], halo_send, halo_recv, (lax.rem(s + 1, n_sp), p)
    )
    stat_copies = [
        copy(stats.at[s], stats.at[s], stat_send.at[k], stat_recv.at[k], (lax.rem(s + k, n_sp), p))
        for k in range(1, n_sp)
    ]
    doc_copy = copy(
        docx.at[:, pl.ds(toks, halo)], docx.at[:, pl.ds(0, halo)], doc_send, doc_recv, (lax.rem(s + 1, n_sp), p)
    )
    for load in inputs[1:5]:
        load.wait()
    values = ext[halo:, :]
    docr = doc[...][None, :].astype(jnp.float32)
    docx[0:1, halo:] = docr
    docc = jnp.transpose(jnp.broadcast_to(docr, (128, toks)))[:, 0:1]
    last = jnp.max(docr, axis=1, keepdims=True)
    first = jnp.min(docr, axis=1, keepdims=True)
    tail = (docr == last).astype(jnp.float32)
    tail_count = jnp.sum(tail, axis=1, keepdims=True)
    sums = dot(jnp.broadcast_to(tail, (8, toks)).astype(jnp.bfloat16), values)
    lane_at = lax.broadcasted_iota(jnp.int32, (8, 128), 1)
    stats[s, :, 0:width] = sums
    stats[s, 0:top, width + 128 :] = ids[...].astype(jnp.float32)
    stats[s, top : 2 * top, width + 128 :] = wts[...]
    stats[s, :, width : width + 128] = jnp.where(lane_at == 0, last, tail_count)
    inputs[0].wait()
    pl.semaphore_wait(barrier, n_sp - 1 + n_x * (n_tp - 1))
    for c in range(cuts):
        for j in steps:
            across(j, c).start()
    for each in stat_copies:
        each.start()
    doc_copy.start()
    halo_copy.start()
    side.start()

    tpos = lax.broadcasted_iota(jnp.int32, (toks, toks), 0)
    spos = lax.broadcasted_iota(jnp.int32, (toks, toks), 1)
    same = ((docc == docr) & (spos <= tpos)).astype(jnp.float32)
    here = jnp.sum(same, axis=1, keepdims=True)
    running = dot(same.astype(jnp.bfloat16), values)
    groups = width // group_width
    for load in inputs[5:]:
        load.wait()
    flat[...] = scales[...].astype(jnp.float32)[None, :]
    tpos = lax.broadcasted_iota(jnp.int32, (toks, toks + halo), 0) + halo
    spos = lax.broadcasted_iota(jnp.int32, (toks, toks + halo), 1)
    away = tpos - spos
    doc_copy.wait_recv()
    halo_copy.wait_recv()
    held = (docc == docx[...]) & (away >= 0) & (spos >= jnp.where(s == 0, halo, 0))
    windows, recents = [], []
    for i in range(groups):
        window = jnp.int32(0)
        for at, size in enumerate(pool_windows):
            window = jnp.where(p * groups + i == at, size, window)
        band = (held & (away < window)).astype(jnp.float32).astype(jnp.bfloat16)
        windows.append(window.astype(jnp.float32))
        recents.append(dot(band, ext[:, i * group_width : (i + 1) * group_width]))
    spread(0)

    for each in stat_copies:
        each.wait_recv()
    spread(1)
    prev_count = jnp.zeros((1, 1), jnp.float32)
    prev_sums = jnp.zeros((1, width), jnp.float32)
    for k in range(n_sp):
        block = stats[k]
        joined = (block[0:1, width : width + 1] == first) & (k < s)
        prev_count = prev_count + jnp.where(joined, block[0:1, width + 1 : width + 2], 0.0)
        prev_sums = prev_sums + jnp.where(joined, block[0:1, 0:width], 0.0)
    carried = docc == first
    length = here + jnp.where(carried, prev_count, 0.0)
    running = running + jnp.where(carried, prev_sums, 0.0)
    doc_mean = running / length
    for i in range(groups):
        g = p * groups + i
        cols = slice(i * group_width, (i + 1) * group_width)
        recent = recents[i] / jnp.minimum(length, windows[i])
        offset = 0.5 * (recent + doc_mean[:, cols]) - values[:, cols].astype(jnp.float32)
        turned = dot(offset.astype(jnp.bfloat16), wg[g])
        scale = flat[0:1, pl.ds(pl.multiple_of(g * group_width, group_width), group_width)]
        mixed[:, cols] = (turned * scale).astype(jnp.bfloat16)
    spread(2)
    for j in steps:
        lend(j).start()

    mix_copies = []
    for k in range(1, n_tp):
        q = lax.rem(p + k, n_tp)
        mix_copies.append(
            copy(
                mixed.at[pl.ds(pl.multiple_of(q * rows, rows), rows)], token_rows.at[p],
                mix_send.at[k], mix_recv.at[k], (s, q),
            )
        )
        mix_copies[-1].start()
    token_rows[p] = mixed[pl.ds(pl.multiple_of(p * rows, rows), rows), :]

    for c in range(3, cuts):
        spread(c)
    side.wait_recv()
    for load in loads:
        load.start()
    for j in steps:
        lend(j).wait_recv()
        mine = mixed[block_rows(lax.rem(p + 2 * j, n_tp)), :]
        total = dot(mine, wb_all[p, :, kept:]) + dot(lent[j], wb_all[partner, :, kept:])
        parts_out[j] = total.astype(jnp.bfloat16)
        part(j).start()
    gather(0)
    gather(1)

    expert_at = [z * n_x * n_tp + lax.rem(x + q // n_tp, n_x) * n_tp + lax.rem(p + q % n_tp, n_tp) for q in range(peers)]
    earlier = lax.broadcasted_iota(jnp.int32, (rows, rows), 0) < lax.broadcasted_iota(jnp.int32, (rows, rows), 1)
    earlier = earlier.astype(jnp.float32).astype(jnp.bfloat16)
    row = lax.broadcasted_iota(jnp.int32, (peers, rows), 0)
    expert = jnp.zeros((peers, rows), jnp.int32)
    for q in range(peers):
        expert = jnp.where(row == q, expert_at[q], expert)
    expert = expert.astype(jnp.float32)
    slot = lax.broadcasted_iota(jnp.int32, (cap, rows), 0).astype(jnp.float32)

    def plan(i):
        zb = near[i]
        meta = stats[zb * n_x + x, :, width + 128 :]
        chosen = jnp.zeros((peers, rows), jnp.float32)
        weight = jnp.zeros((peers, rows), jnp.float32)
        for a in range(top):
            hit = meta[a : a + 1, :] == expert
            chosen = chosen + jnp.where(hit, 1.0, 0.0)
            weight = weight + jnp.where(hit, meta[top + a : top + a + 1, :], 0.0)
        key = jnp.where(chosen > 0.0, dot(chosen.astype(jnp.bfloat16), earlier), -1.0)
        for q in range(peers):
            taken = slot == key[q : q + 1, :]
            pick[zb, seat(q), :] = jnp.where(taken, 1.0, 0.0).astype(jnp.bfloat16)
            full = jnp.where(taken, weight[q : q + 1, :], 0.0)
            high = full.astype(jnp.bfloat16)
            share[zb, seat(q), 0:rows] = high
            share[zb, seat(q), rows:] = (full - high.astype(jnp.float32)).astype(jnp.bfloat16)

    plan(0)
    gather(2)
    for c in range(3, cuts):
        gather(c)
    for each in mix_copies:
        each.wait_recv()
    branch = alpha_mix * resid[...].astype(jnp.float32)
    for k in (p, partner):
        branch = branch + dot(token_rows[k], wb_all[k])
    for c in range(cuts):
        for j in steps:
            for o in range(n_x):
                onward(j, o, c).wait_recv()
    left, right = branch[:, :kept], branch[:, kept:]
    for j in steps:
        for k in (slot_of(j), partner + slot_of(j) - p):
            left = left + dot(token_rows[k], wb_all[k, :, :kept])
    for j in steps:
        part(j).wait_recv()
        right = right + parts_in[j].astype(jnp.float32)
    branch = jnp.concatenate([left, right], axis=1)
    blocks[z] = layer_norm(branch, ngain[...][None, :]).astype(jnp.bfloat16)
    for c in range(chunks):
        relay(z, c)

    dispatch(0)
    for i in range(1, n_z):
        plan(i)
    shared()
    for i in range(1, n_z):
        receive(i)
        dispatch(i)
    last = n_z - 1
    for i in range(last, 0, -1):
        experts(i)
    combine(last)
    pass_on(last)
    experts(0)
    for i in range(last - 1, 0, -1):
        combine(i)
        pass_on(i)
    combine(0)
    for c in range(chunks):
        take(0, z, c, z > 0)
        take(1, z, c, z + 1 < n_z)
    out_ref[...] = layer_norm(column[z], fgain[...][None, :]).astype(jnp.bfloat16)

    for zb in range(n_z):
        for c in range(chunks):
            src = blocks.at[zb, :, lane(c)]

            @pl.when(rises(zb))
            def _():
                up(src, zb, c).wait_send()

            @pl.when(sinks(zb))
            def _():
                down(src, zb, c).wait_send()

    for i in range(1, n_z):
        for c in range(chunks):
            link(0, near[i], c).wait_send()
    for i in range(n_z):
        for q in range(1, peers):
            go(i, q).wait_send()
            back(i, q).wait_send()
    halo_copy.wait_send()
    doc_copy.wait_send()
    for j in steps:
        lend(j).wait_send()
        part(j).wait_send()
    side.wait_send()
    for each in stat_copies + mix_copies:
        each.wait_send()
    for c in range(cuts):
        for j in steps:
            across(j, c).wait_send()
            onward(j, 0, c).wait_send()
            for o in range(1, n_x):
                along(j, o, c).wait_send()
                onward(j, o, c).wait_send()


def local(
    n_sp, n_tp,
    resid, pool_in, doc_ids, w_group, pool_scale, w_branch, norm_gain, route_ids, route_wts,
    w_exp_gate, w_exp_up, w_exp_down, w_sh_gate, w_sh_up, w_sh_down, final_gain,
):
    toks, width = pool_in.shape
    rows, model = resid.shape
    depth = w_branch.shape[0]
    top = route_ids.shape[1]
    cap = 2 * rows * top // (n_sp * n_tp)
    n_x = max(k for k in range(1, n_sp + 1) if n_sp % k == 0 and k * k <= n_sp)
    n_z = n_sp // n_x
    ff = w_sh_gate.shape[1]
    vmem, hbm = pl.BlockSpec(memory_space=pltpu.VMEM), pl.BlockSpec(memory_space=pl.ANY)
    dma = pltpu.SemaphoreType.DMA
    bf16, f32 = jnp.bfloat16, jnp.float32
    peers = n_x * n_tp
    seats = pltpu.VMEM((n_z, peers * cap, model), bf16)
    block = (rows, model)
    wide, tall = pltpu.VMEM((model, ff), bf16), pltpu.VMEM((ff, model), bf16)
    hops = n_tp // 2
    summed = model - int(model * sent_part) // 128 * 128
    return pl.pallas_call(
        functools.partial(layer_kernel, n_sp, n_tp, n_x, cap, top),
        out_shape=jax.ShapeDtypeStruct(block, bf16),
        in_specs=[hbm] * 16,
        out_specs=vmem,
        scratch_shapes=[
            pltpu.VMEM((halo + toks, width), bf16),
            pltpu.VMEM(doc_ids.shape, jnp.int32),
            pltpu.VMEM((1, halo + toks), f32),
            pltpu.VMEM(w_group.shape, bf16),
            pltpu.VMEM(pool_scale.shape, bf16),
            pltpu.VMEM((1, *pool_scale.shape), f32),
            pltpu.VMEM(block, bf16),
            pltpu.VMEM((model,), bf16),
            pltpu.VMEM((top, rows), jnp.int32),
            pltpu.VMEM((top, rows), f32),
            pltpu.VMEM((model,), bf16),
            pltpu.VMEM((n_sp, 8, width + 128 + rows), f32),
            pltpu.VMEM((toks, width), bf16),
            pltpu.VMEM((n_tp, rows, width), bf16),
            pltpu.VMEM((n_tp, depth, model), bf16),
            pltpu.VMEM((hops, rows, width), bf16),
            pltpu.VMEM((hops, rows, summed), bf16), pltpu.VMEM((hops, rows, summed), bf16),
            wide, wide, tall, wide, wide, tall,
            pltpu.VMEM((n_z, *block), bf16),
            seats, seats, seats,
            pltpu.VMEM((n_z, *block), f32),
            pltpu.VMEM((n_z, *block), bf16),
            pltpu.VMEM((2, n_z, *block), bf16),
            pltpu.VMEM(block, f32),
            pltpu.VMEM((n_z, peers * cap, rows), bf16), pltpu.VMEM((n_z, peers * cap, 2 * rows), bf16),
            dma((10,)), dma((n_sp,)), dma((n_sp,)), dma, dma, dma, dma, dma((n_tp,)), dma((n_tp,)),
            dma((hops, wb_cuts)), dma((hops, wb_cuts)),
            dma((hops, n_x, wb_cuts)), dma((hops, n_x, wb_cuts)), dma, dma,
            dma((hops, n_x, wb_cuts)), dma((hops, n_x, wb_cuts)),
            dma((hops,)), dma((hops,)), dma((hops,)), dma((hops,)),
            dma((6,)), dma((n_z, chunks)), dma((n_z, chunks)), dma((n_z, chunks)),
            dma((n_z, peers)), dma((n_z, peers)), dma((n_z, peers)), dma((n_z, peers)),
            dma((n_z, chunks)), dma((2, n_z, chunks)),
        ],
        compiler_params=pltpu.CompilerParams(
            collective_id=0, has_side_effects=True, vmem_limit_bytes=62 << 20
        ),
        name="pool_and_experts",
    )(
        pool_in, doc_ids, w_group, pool_scale, w_branch, resid, norm_gain, route_ids.T, route_wts.T,
        w_exp_gate, w_exp_up, w_exp_down, w_sh_gate, w_sh_up, w_sh_down, final_gain,
    )


def solution(mesh):
    both = P(("sp", "tp"), None)
    stack = P(("sp", "tp"), None, None)
    placed = (
        both, P("sp", "tp"), P("sp"), P(), P(), P("tp", None), P(), both, both,
        stack, stack, stack, P(), P(), P(), P(),
    )
    return jax.shard_map(
        functools.partial(local, mesh.shape["sp"], mesh.shape["tp"]),
        mesh=mesh, in_specs=placed, out_specs=both, check_vma=False,
    )
```
